32 devices in a mesh: sp: 8 (over z, x), tp: 4 (over y, core).
Axes of the slice: x: 2, y: 2, z: 4, core: 2. Of those that a mesh axis runs over, the one named last changes fastest.
Arguments:
- cotangent: bfloat16 [2048, 2048], P('sp', 'tp'), may hold values from -6 to 6
- moe_input: bfloat16 [2048, 2048], P('sp', 'tp'), may hold values from -6 to 6
- routes: int32 [2048, 2], P('sp'), may hold values from 0 to 7, all different within a row; in each aligned block of 256 rows (0 to 255, 256 to 511, ...) at most 96 rows name the same one
- gates: float32 [2048, 2], P('sp'), may hold values from 0.1 to 1
- w_gate: bfloat16 [8, 2048, 2048], P('sp', None, 'tp'), may hold values from -0.125 to 0.125
- w_up: bfloat16 [8, 2048, 2048], P('sp', None, 'tp'), may hold values from -0.125 to 0.125
- w_down: bfloat16 [8, 2048, 2048], P('sp', 'tp'), may hold values from -0.125 to 0.125
- out_proj: bfloat16 [1024, 2048], P('tp'), may hold values from -0.1875 to 0.1875
- conv_in: bfloat16 [1024, 2048], P('tp', 'sp'), may hold values from -6 to 6
- branch: bfloat16 [1024, 2048], P('tp', 'sp'), may hold values from -6 to 6
- state_before: float32 [1024, 2048], P('tp', 'sp'), may hold values from -6 to 6
- state_after: float32 [1024, 2048], P('tp', 'sp'), may hold values from -6 to 6
- jump: float32 [1024, 2048], P('tp', 'sp'), may hold values from -2 to 0, as said below
- recur_weight: bfloat16 [2, 16, 64, 64], P(None, 'tp'), may hold values from -0.75 to 0.75
- input_weight: bfloat16 [2, 16, 64, 64], P(None, 'tp'), may hold values from -0.75 to 0.75
- lam: float32 [2, 1024], P(None, 'tp')
Outputs:
- gate_grad: bfloat16 [8, 2048, 2048], P('sp', None, 'tp')
- up_grad: bfloat16 [8, 2048, 2048], P('sp', None, 'tp')
- down_grad: bfloat16 [8, 2048, 2048], P('sp', 'tp')
- residual_grad: bfloat16 [2048, 2048], P('sp', 'tp')
- out_proj_grad: float32 [1024, 2048], P('tp', 'sp')
- conv_grad: float32 [1024, 2048], P('tp', 'sp')
- branch_grad: float32 [1024, 2048], P('tp', 'sp')
The draws below stay inside these ranges and needn't reach their ends.
Inputs may be any that keep to these rules, and one draw needn't show every extreme that they name: `routes`: each token names 2 different experts. Among the tokens of one index of sp (aligned blocks of 256 rows) no expert is named more than 96 times, a bound that some block reaches. `jump`: every entry is at most -1 / 20480.
All inputs are finite; a program needn't handle non-finite values.
Results may differ from the reference program's by a relative error of at most 0.02.
Values may be sent and summed in bfloat16 or wider, within the bound.
No kernel may reach another device: no remote copies, remote signals or barrier semaphores. Data moves between devices by JAX's collectives and lax.ppermute only.
A program may use at most 128 MiB of HBM per device.

```python
import math
import jax
import jax.numpy as jnp
import numpy as np
from jax import lax

D = 2048
RECURRENT_WIDTH = 1024
BW = 64
BLOCKS = 16
FFE = 2048
TOP = 2
TOK_DEV = 256
EXPERTS = 8
SEQUENCE_TOKENS = 2048
CAP = 96
N_SP = 8
N_TP = 4


def draw_lam(key, part):
    k_fast, k_span, k_slow = jax.random.split(jax.random.fold_in(key, 11), 3)
    fast_share = 0.5
    is_fast = jax.random.uniform(k_fast, (2, RECURRENT_WIDTH), jnp.float32) < fast_share
    fast_len = jax.random.uniform(k_span, (2, RECURRENT_WIDTH), jnp.float32, 30.0, 100.0)
    slow_len = SEQUENCE_TOKENS * jax.random.uniform(k_slow, (2, RECURRENT_WIDTH), jnp.float32, 1.0, 2.0)
    length = jnp.where(is_fast, fast_len, slow_len)
    step_rate = 2.0 / (8.0 * length)
    return -jnp.log(jnp.expm1(step_rate))


def draw_jump(key, part):
    folded = jax.random.fold_in(key, 23)
    k_rate, k_cell, random_location, random_extent = jax.random.split(folded, 4)
    blocks = SEQUENCE_TOKENS // TOK_DEV
    block_rate = jnp.exp(jax.random.uniform(k_rate, (blocks,), jnp.float32, math.log(0.2), math.log(0.8)))
    cell_multiplier = jnp.exp(jax.random.uniform(k_cell, (RECURRENT_WIDTH, SEQUENCE_TOKENS), jnp.float32, math.log(0.5), math.log(2.0)))
    token_position = jnp.arange(SEQUENCE_TOKENS, dtype=jnp.int32)
    position_values = jnp.repeat(block_rate, TOK_DEV) / SEQUENCE_TOKENS
    spike_offset = jax.random.randint(random_location, (2,), 0, SEQUENCE_TOKENS)
    spike_mask = ((token_position == spike_offset[0]) | (token_position == spike_offset[1])).astype(jnp.float32)[None, :]
    spike_extent = jnp.log(jax.random.uniform(random_extent, (RECURRENT_WIDTH, 1), jnp.float32, 0.55, 0.8))
    return -position_values[None, :] * cell_multiplier + spike_mask * spike_extent


def spiked(values, own_key, source, target, parts, factor):
    def block_of(position):
        return (jnp.arange(values.shape[position]) // (values.shape[position] // parts)).reshape((-1,) + (1,) * (values.ndim - 1 - position))

    first = jax.random.permutation(own_key, parts)[block_of(target)]
    second = (block_of(target) + parts // 2) % parts
    return jnp.where((block_of(source) == first) | (block_of(source) == second), factor * values, values)


def levels(rng, extent, cuts, least, high):
    loudness = 1.0
    for dim, parts in cuts:
        steps = jax.random.uniform(jax.random.fold_in(jax.random.fold_in(rng, 6), dim), (parts,), jnp.float32, least / len(cuts), high / len(cuts))
        loudness = loudness * jnp.repeat(jnp.exp(steps), extent[dim] // parts).reshape((-1,) + (1,) * (len(extent) - 1 - dim))
    return loudness


def assign_block(rng, own, number, rows, number_of, top, most, skew):
    sequence = jax.random.permutation(rng, number_of)
    heavy_load, ordinary = load_shares(number_of, rows * top, most, skew, True), load_shares(number_of, rows * top, most, skew, False)
    places = jnp.arange(number_of)

    def named(sizes, turn):
        used = int((sizes > 0).sum())
        fixed = max(1, used // 4)
        shifted = fixed + (places - fixed + turn * (used - fixed)) % max(1, number_of - fixed)
        return jnp.zeros((number_of,), jnp.int32).at[sequence[jnp.where(places < fixed, places, shifted)]].set(jnp.asarray(sizes, jnp.int32))

    sizes = jnp.where(number % 4 == 0, named(heavy_load, number // 4), named(ordinary, number - number // 4 - 1))
    mixed = jax.random.permutation(jax.random.fold_in(own, 3), number_of)
    donor, receiver = mixed[0:number_of // 2 * 2:2], mixed[1:number_of // 2 * 2:2]
    margin = jnp.minimum(sizes[donor] - 1, most - sizes[receiver]) // 2
    margin = jnp.where((donor == sequence[0]) | (receiver == sequence[0]) | (sizes[receiver] == 0), 0, jnp.maximum(margin, 0))
    shifted = jax.random.randint(jax.random.fold_in(own, 4), (number_of // 2,), 0, 1 << 20) % (margin + 1)
    sizes = sizes.at[donor].add(-shifted).at[receiver].add(shifted)
    items = jnp.searchsorted(jnp.cumsum(sizes), jnp.arange(rows * top), side="right").astype(jnp.int32)
    listing = items.reshape(top, rows).T
    listing = listing[jax.random.permutation(jax.random.fold_in(own, 1), rows)]
    turn = jax.random.randint(jax.random.fold_in(own, 2), (rows, 1), 0, top)
    return jnp.take_along_axis(listing, (jnp.arange(top)[None, :] + turn) % top, axis=1)


def load_shares(number_of, total, most, lean, full):
    portions = [(1 << 20) // math.isqrt(grade ** lean) + 1 for grade in range(1, number_of + 1)]
    largest = most if full else min(most, max(-(-total // number_of), total * portions[0] // sum(portions)))
    least = 1 if total - largest >= number_of - 1 else 0
    given, surplus = [largest] + [least] * (number_of - 1), total - largest - least * (number_of - 1)
    while surplus > 0:
        free = [i for i in range(1, number_of) if given[i] < largest] or [i for i in range(1, number_of) if given[i] < most]
        whole, remaining = sum([portions[i] for i in free]), surplus
        for i in free:
            extra = min(most - given[i], max(1, remaining * portions[i] // whole), surplus)
            given[i] = given[i] + extra
            surplus = surplus - extra
    return np.array(given)


def bell_draw(rng, shape, spread, limit, cuts=(), kind=jnp.bfloat16):
    array = spread * jax.random.normal(rng, shape, jnp.float32)
    if cuts:
        array = array * levels(rng, shape, cuts, -0.22, 0.18)
    return jnp.clip(array, -limit, limit).astype(kind)


def gaussian_with(key, dims, scale, most, cuts, heavy, kind=jnp.bfloat16):
    array = scale * jax.random.normal(key, dims, jnp.float32)
    if cuts:
        array = array * levels(key, dims, cuts, -0.22, 0.18)
    return jnp.clip(spiked(array, jax.random.fold_in(key, 3), *heavy), -most, most).astype(kind)


def setup_inputs(seed: int = 0) -> dict:
    key_list = jax.random.split(jax.random.key(seed), 17)
    cotangent = gaussian_with(key_list[0], (SEQUENCE_TOKENS, D), 1.0, 6.0, ((0, 8), (1, 4)), (0, 1, 8, 2.0))
    moe_input = bell_draw(key_list[1], (SEQUENCE_TOKENS, D), 1.0, 6.0, ((0, 8), (1, 4)))
    routes_keys = jax.random.split(jax.random.fold_in(key_list[2], 1), SEQUENCE_TOKENS // TOK_DEV)
    routes_turns = jax.random.permutation(jax.random.fold_in(key_list[2], 3), SEQUENCE_TOKENS // TOK_DEV)
    routes = jax.vmap(lambda own, number: assign_block(jax.random.fold_in(key_list[2], 2), own, number, TOK_DEV, EXPERTS, TOP, CAP, 1))(routes_keys, routes_turns).reshape((SEQUENCE_TOKENS, TOP))
    gates = jnp.clip(0.1 + 0.9 * jax.random.uniform(key_list[3], (SEQUENCE_TOKENS, TOP), jnp.float32) ** levels(key_list[3], (SEQUENCE_TOKENS, TOP), ((0, 8),), -0.2, 0.2), 0.1, 1.0)
    w_gate = bell_draw(key_list[4], (EXPERTS, D, FFE), D ** -0.5, 0.125, ((0, 8), (2, 4)))
    w_up = bell_draw(key_list[5], (EXPERTS, D, FFE), D ** -0.5, 0.125, ((0, 8), (2, 4)))
    w_down = bell_draw(key_list[6], (EXPERTS, FFE, D), FFE ** -0.5, 0.125, ((0, 8), (1, 4)))
    out_proj = bell_draw(key_list[7], (RECURRENT_WIDTH, D), RECURRENT_WIDTH ** -0.5, 0.1875, ((0, 4),))
    conv_in = bell_draw(key_list[8], (RECURRENT_WIDTH, SEQUENCE_TOKENS), 1.0, 6.0, ((0, 4), (1, 8)))
    branch = bell_draw(key_list[9], (RECURRENT_WIDTH, SEQUENCE_TOKENS), 1.0, 6.0, ((0, 4), (1, 8)))
    state_before = bell_draw(key_list[10], (RECURRENT_WIDTH, SEQUENCE_TOKENS), 1.0, 6.0, ((0, 4), (1, 8)), jnp.float32)
    state_after = bell_draw(key_list[11], (RECURRENT_WIDTH, SEQUENCE_TOKENS), 1.0, 6.0, ((0, 4), (1, 8)), jnp.float32)
    jump = draw_jump(jax.random.fold_in(key_list[16], 71), 0)
    recur_weight = bell_draw(key_list[13], (2, BLOCKS, BW, BW), BW ** -0.5, 0.75, ((1, 4),))
    input_weight = bell_draw(key_list[14], (2, BLOCKS, BW, BW), BW ** -0.5, 0.75, ((1, 4),))
    lam = draw_lam(jax.random.fold_in(key_list[16], 71), 0)
    return {"cotangent": cotangent, "moe_input": moe_input, "routes": routes, "gates": gates, "w_gate": w_gate, "w_up": w_up, "w_down": w_down, "out_proj": out_proj, "conv_in": conv_in, "branch": branch, "state_before": state_before, "state_after": state_after, "jump": jump, "recur_weight": recur_weight, "input_weight": input_weight, "lam": lam}


decay_scale = 8.0

def silu_parts(pre_act):
    sigmoid_val = jax.nn.sigmoid(pre_act)
    return (pre_act * sigmoid_val, sigmoid_val * (1.0 + pre_act * (1.0 - sigmoid_val)))

def block_map(values, weight):
    return jnp.einsum('nit,nij->njt', values.astype(jnp.float32), weight.astype(jnp.float32), precision=lax.Precision.HIGHEST)

def block_back(gradient, weight):
    return jnp.einsum('njt,nij->nit', gradient, weight.astype(jnp.float32), precision=lax.Precision.HIGHEST)

def gate_values(conv_in, weight_r, weight_i, lam_row, jump):
    channels, length = conv_in.shape
    shaped = conv_in.reshape(weight_r.shape[0], weight_r.shape[1], length)
    recur_gate = jax.nn.sigmoid(block_map(shaped, weight_r).reshape(channels, length))
    inward = jax.nn.sigmoid(block_map(shaped, weight_i).reshape(channels, length))
    speed_row = decay_scale * jax.nn.softplus(-lam_row)[:, None]
    log_decay = -speed_row * recur_gate + jump
    retain = jnp.exp(log_decay)
    root_term = jnp.sqrt(-jnp.expm1(2.0 * log_decay))
    conv_wide = conv_in.astype(jnp.float32)
    return (recur_gate, inward, speed_row, retain, root_term, conv_wide)

def gate_backward(pieces, decay_grad, drive_grad, weight_r, weight_i):
    recur_gate, inward, speed_row, retain, root_term, conv_wide = pieces
    channels, length = conv_wide.shape
    shape_three = (weight_r.shape[0], weight_r.shape[1], length)
    log_grad = decay_grad * retain - drive_grad * inward * conv_wide * retain * retain / root_term
    recur_grad = log_grad * -speed_row * recur_gate * (1.0 - recur_gate)
    inward_grad = drive_grad * root_term * conv_wide * inward * (1.0 - inward)
    direct = drive_grad * root_term * inward
    back_r = block_back(recur_grad.reshape(shape_three), weight_r)
    back_i = block_back(inward_grad.reshape(shape_three), weight_i)
    return direct + (back_r + back_i).reshape(channels, length)

def combine_pair(earlier, latter):
    return (earlier[0] * latter[0], latter[0] * earlier[1] + latter[1])

def expert_terms(routed_rows, routed_grads, gate_weight, up_weight, down_weight):
    pre_gate = jnp.dot(routed_rows, gate_weight, preferred_element_type=jnp.float32)
    pre_up = jnp.dot(routed_rows, up_weight, preferred_element_type=jnp.float32)
    silu_val, silu_slope = silu_parts(pre_gate)
    activation = (silu_val * pre_up).astype(jnp.bfloat16)
    act_grad = jnp.dot(routed_grads, down_weight.T, preferred_element_type=jnp.float32)
    up_hidden = (act_grad * silu_val).astype(jnp.bfloat16)
    gate_hidden = (act_grad * pre_up * silu_slope).astype(jnp.bfloat16)
    down_acc = jnp.dot(activation.T, routed_grads, preferred_element_type=jnp.float32)
    gate_acc = jnp.dot(routed_rows.T, gate_hidden, preferred_element_type=jnp.float32)
    up_acc = jnp.dot(routed_rows.T, up_hidden, preferred_element_type=jnp.float32)
    return (gate_hidden, up_hidden, gate_acc, up_acc, down_acc)

def reference(cotangent, moe_input, routes, gates, w_gate, w_up, w_down, out_proj, conv_in, branch, state_before, state_after, jump, recur_weight, input_weight, lam):
    per_token = routes.shape[1]
    routed = routes.reshape(-1)
    pair_total = routed.shape[0]
    scaled = (cotangent.astype(jnp.float32)[:, None, :] * gates[:, :, None]).astype(jnp.bfloat16)
    scaled = scaled.reshape(pair_total, D)
    copies = jnp.broadcast_to(moe_input[:, None, :], (SEQUENCE_TOKENS, per_token, D)).reshape(pair_total, D)
    zero_row = jnp.zeros((1, D), jnp.bfloat16)
    padded_rows = jnp.concatenate([copies, zero_row], axis=0)
    padded_grads = jnp.concatenate([scaled, zero_row], axis=0)
    buffer_rows = N_SP * CAP
    per_dev = FFE // N_TP

    def one_expert(returned, inputs):
        gate_weight, up_weight, down_weight, expert = inputs
        chosen = jnp.nonzero(routed == expert, size=buffer_rows, fill_value=pair_total)[0].astype(jnp.int32)
        routed_rows = padded_rows[chosen]
        routed_grads = padded_grads[chosen]
        gate_hidden, up_hidden, gate_acc, up_acc, down_acc = expert_terms(routed_rows, routed_grads, gate_weight, up_weight, down_weight)
        split_gate = jnp.einsum('rkf,dkf->krd', gate_hidden.astype(jnp.float32).reshape(buffer_rows, N_TP, per_dev), gate_weight.astype(jnp.float32).reshape(D, N_TP, per_dev), precision=lax.Precision.HIGHEST)
        split_up = jnp.einsum('rkf,dkf->krd', up_hidden.astype(jnp.float32).reshape(buffer_rows, N_TP, per_dev), up_weight.astype(jnp.float32).reshape(D, N_TP, per_dev), precision=lax.Precision.HIGHEST)
        partial_value = (split_gate + split_up).astype(jnp.bfloat16)
        partial_value = lax.optimization_barrier(partial_value)
        row_grad = lax.optimization_barrier(jnp.sum(partial_value.astype(jnp.float32), axis=0)).astype(jnp.bfloat16)
        returned = returned.at[chosen].set(row_grad)
        return (returned, (gate_acc.astype(jnp.bfloat16), up_acc.astype(jnp.bfloat16), down_acc.astype(jnp.bfloat16)))
    start = jnp.zeros((pair_total + 1, D), jnp.bfloat16)
    returned, grads_all = lax.scan(one_expert, start, (w_gate, w_up, w_down, jnp.arange(EXPERTS, dtype=jnp.int32)))
    gate_grad, up_grad, down_grad = grads_all
    backward_rows = returned[:pair_total].reshape(SEQUENCE_TOKENS, per_token, D)
    residual_grad = (cotangent.astype(jnp.float32) + lax.optimization_barrier(jnp.sum(backward_rows.astype(jnp.float32), axis=1))).astype(jnp.bfloat16)
    mix_grad = jnp.dot(out_proj, residual_grad.T, preferred_element_type=jnp.float32)
    pieces_fwd = gate_values(conv_in, recur_weight[0], input_weight[0], lam[0], jump)
    pieces_bwd = gate_values(conv_in, recur_weight[1], input_weight[1], lam[1], jump)
    drive_fwd = pieces_fwd[4] * pieces_fwd[1] * pieces_fwd[5]
    drive_bwd = pieces_bwd[4] * pieces_bwd[1] * pieces_bwd[5]
    lru_out = pieces_fwd[3] * state_before + drive_fwd + pieces_bwd[3] * state_after + drive_bwd
    gelu_val, gelu_back = jax.vjp(jax.nn.gelu, branch.astype(jnp.float32))
    mix = (lru_out * gelu_val).astype(jnp.bfloat16)
    out_proj_grad = jnp.dot(mix, residual_grad, preferred_element_type=jnp.float32)
    lru_grad = mix_grad * gelu_val
    branch_grad = gelu_back(mix_grad * lru_out)[0]
    decay_fwd = pieces_fwd[3]
    decay_bwd = pieces_bwd[3]
    carried_fwd = lax.associative_scan(combine_pair, (decay_fwd, decay_fwd * lru_grad), reverse=True, axis=1)[1]
    carried_bwd = lax.associative_scan(combine_pair, (decay_bwd, decay_bwd * lru_grad), axis=1)[1]
    zeros_col = jnp.zeros((RECURRENT_WIDTH, 1), jnp.float32)
    delta_fwd = lru_grad + jnp.concatenate([carried_fwd[:, 1:], zeros_col], axis=1)
    delta_bwd = lru_grad + jnp.concatenate([zeros_col, carried_bwd[:, :-1]], axis=1)
    conv_grad = gate_backward(pieces_fwd, delta_fwd * state_before, delta_fwd, recur_weight[0], input_weight[0])
    conv_grad = conv_grad + gate_backward(pieces_bwd, delta_bwd * state_after, delta_bwd, recur_weight[1], input_weight[1])
    return (gate_grad, up_grad, down_grad, residual_grad, out_proj_grad, conv_grad, branch_grad)
```

```python
import functools

import jax
import jax.numpy as jnp
from jax import lax
from jax.experimental import pallas as pl
from jax.experimental.pallas import tpu as pltpu
from jax.sharding import PartitionSpec as P


decay_scale = 8.0
groups_of_sources = 2
f32 = jnp.float32
bf16 = jnp.bfloat16

nn = (((1,), (0,)), ((), ()))
nt = (((1,), (1,)), ((), ()))
tn = (((0,), (0,)), ((), ()))


def dot(a, b, dims):
    return lax.dot_general(a, b, dims, preferred_element_type=f32)


def call(kernel, inputs, outs, scratch=(), flops=0, scalars=1, name=None):
    moved = sum(a.size * a.dtype.itemsize for a in inputs) + sum(
        o.size * o.dtype.itemsize for o in outs
    )
    specs = [pl.BlockSpec(memory_space=pltpu.SMEM)] * scalars
    specs += [pl.BlockSpec(memory_space=pltpu.VMEM)] * (len(inputs) - scalars)
    return pl.pallas_call(
        kernel,
        out_shape=tuple(outs),
        in_specs=specs,
        out_specs=tuple(pl.BlockSpec(memory_space=pltpu.VMEM) for _ in outs),
        scratch_shapes=list(scratch),
        cost_estimate=pl.CostEstimate(
            flops=int(flops), bytes_accessed=int(moved), transcendentals=0
        ),
        compiler_params=pltpu.CompilerParams(vmem_limit_bytes=48 * 1024 * 1024),
        name=name,
    )(*inputs)


def shape(dims, kind):
    return jax.ShapeDtypeStruct(dims, kind)


def pack_kernel(experts, capacity, place_ref, routes_ref, gates_ref, rows_ref, cot_ref, *out_refs):
    position_ref, blocks = out_refs[0], out_refs[1:]
    tokens, top = routes_ref.shape
    width = rows_ref.shape[1]
    lanes = max(128, experts)
    named = lax.broadcasted_iota(jnp.int32, (tokens, lanes), 1)
    routes = routes_ref[...]
    picks = [routes[:, k : k + 1] for k in range(top)]
    onehots = [(pick == named).astype(f32) for pick in picks]
    both = functools.reduce(jnp.add, onehots).astype(bf16)
    before = (
        lax.broadcasted_iota(jnp.int32, (tokens, tokens), 0)
        > lax.broadcasted_iota(jnp.int32, (tokens, tokens), 1)
    ).astype(f32).astype(bf16)
    earlier = dot(before, both, nn)
    positions = [
        jnp.sum(earlier * onehot, axis=1, keepdims=True).astype(jnp.int32) for onehot in onehots
    ]
    for k in range(top):
        position_ref[:, k : k + 1] = positions[k]
    rows = rows_ref[...]
    cot = cot_ref[...].astype(f32)
    scaled = [(cot * gates_ref[:, k : k + 1]).astype(bf16) for k in range(top)]
    slot = lax.broadcasted_iota(jnp.int32, (tokens, capacity), 1)
    for s in range(experts):
        expert = place_ref[0] ^ s
        selects = [
            (jnp.where(pick == expert, position, -1) == slot).astype(f32).astype(bf16)
            for pick, position in zip(picks, positions)
        ]
        blocks[s][:, :width] = dot(functools.reduce(jnp.add, selects), rows, tn).astype(bf16)
        grads = functools.reduce(jnp.add, [dot(sel, sc, tn) for sel, sc in zip(selects, scaled)])
        blocks[s][:, width:] = grads.astype(bf16)


def combine_kernel(experts, place_ref, routes_ref, position_ref, cot_ref, *refs):
    blocks, out_ref = refs[:experts], refs[experts]
    tokens, top = routes_ref.shape
    capacity = blocks[0].shape[0]
    slot = lax.broadcasted_iota(jnp.int32, (tokens, capacity), 1)
    total = cot_ref[...].astype(f32)
    added = jnp.zeros_like(total)
    for s in range(experts):
        expert = place_ref[0] ^ s
        select = functools.reduce(
            jnp.add,
            [
                (
                    jnp.where(routes_ref[:, k : k + 1] == expert, position_ref[:, k : k + 1], -1)
                    == slot
                ).astype(f32)
                for k in range(top)
            ],
        ).astype(bf16)
        added = added + dot(select, blocks[s][...], nn)
    out_ref[...] = (total + added).astype(bf16)


def bit_order(count):
    bits = count.bit_length() - 1
    return [int(format(i, "0%db" % bits)[::-1], 2) if bits else 0 for i in range(count)]


def expert_kernel(ranks, place_ref, *refs):
    parts = refs[:ranks]
    gate_ref, up_ref, down_ref = refs[ranks : ranks + 3]
    keep_ref, send_ref, act_ref, gate_hid_ref, up_hid_ref = refs[ranks + 3 :]
    width = parts[0].shape[1] // 2
    hidden = gate_ref.shape[1]
    tile = min(256, hidden)
    place = place_ref[0]
    offsets = [pl.multiple_of((place ^ r) * width, width) for r in range(ranks)]
    for h in range(hidden // tile):
        cols = slice(h * tile, (h + 1) * tile)
        pre_gate = pre_up = act_grad = None
        for r in range(ranks):
            rows = parts[r][:, :width]
            grads = parts[r][:, width:]
            where = pl.ds(offsets[r], width)
            one = dot(rows, gate_ref[where, cols], nn)
            two = dot(rows, up_ref[where, cols], nn)
            three = dot(grads, down_ref[cols, where], nt)
            pre_gate = one if r == 0 else pre_gate + one
            pre_up = two if r == 0 else pre_up + two
            act_grad = three if r == 0 else act_grad + three
        sig = 1.0 / (1.0 + jnp.exp(-pre_gate))
        silu = pre_gate * sig
        slope = sig * (1.0 + pre_gate * (1.0 - sig))
        act_ref[:, cols] = (silu * pre_up).astype(bf16)
        up_hid_ref[:, cols] = (act_grad * silu).astype(bf16)
        gate_hid_ref[:, cols] = (act_grad * pre_up * slope).astype(bf16)
    gate_hid = gate_hid_ref[...]
    up_hid = up_hid_ref[...]
    half = ranks // 2
    for i, r in enumerate(bit_order(ranks)):
        where = pl.ds(offsets[r], width)
        part = dot(gate_hid, gate_ref[where, :], nt) + dot(up_hid, up_ref[where, :], nt)
        if i < half:
            keep_ref[i] = part.astype(bf16)
        else:
            send_ref[i - half] = part.astype(bf16)


def weight_kernel(ranks, groups, place_ref, *refs):
    parts = [refs[g * ranks : (g + 1) * ranks] for g in range(groups)]
    rest = refs[groups * ranks :]
    acts, gate_hids, up_hids = rest[:groups], rest[groups : 2 * groups], rest[2 * groups : 3 * groups]
    gate_out, up_out, down_out, gate_buf, up_buf, down_buf, sems = rest[3 * groups :]
    width = parts[0][0].shape[1] // 2
    place = place_ref[0]
    copies = []
    for r in range(ranks):
        where = pl.ds(pl.multiple_of((place ^ r) * width, width), width)
        for j, (hids, buf, out) in enumerate(
            ((gate_hids, gate_buf, gate_out), (up_hids, up_buf, up_out))
        ):
            total = None
            for g in range(groups):
                one = dot(parts[g][r][:, :width], hids[g][...], tn)
                total = one if g == 0 else total + one
            buf[r] = total.astype(bf16)
            copy = pltpu.make_async_copy(buf.at[r], out.at[where, :], sems.at[j, r])
            copy.start()
            copies.append(copy)
        total = None
        for g in range(groups):
            one = dot(acts[g][...], parts[g][r][:, width:], tn)
            total = one if g == 0 else total + one
        down_buf[r] = total.astype(bf16)
        copy = pltpu.make_async_copy(down_buf.at[r], down_out.at[:, where], sems.at[2, r])
        copy.start()
        copies.append(copy)
    for copy in copies:
        copy.wait()


def shifted(values, step, reverse, fill):
    length = values.shape[1]
    lane = lax.broadcasted_iota(jnp.int32, values.shape, 1)
    if reverse:
        return jnp.where(lane < length - step, pltpu.roll(values, length - step, 1), fill)
    return jnp.where(lane >= step, pltpu.roll(values, step, 1), fill)


def one_less_exp(power, value):
    series = 1.0 + power * (1.0 / 7.0)
    for term in range(6, 1, -1):
        series = 1.0 + power * (1.0 / term) * series
    return jnp.where(power > -0.35, -power * series, 1.0 - value)


def gates_kernel(
    conv_ref, branch_ref, before_ref, after_ref, jump_ref, maps_ref, speed_ref,
    mix_ref, gelu_ref, back_ref, decay_ref, direct_ref, recur_ref, inward_ref,
):
    blocks, size = maps_ref.shape[0], maps_ref.shape[1]
    for b in range(blocks):
        part = slice(b * size, (b + 1) * size)
        conv_in = conv_ref[part, :]
        conv = conv_in.astype(f32)
        jump = jump_ref[part, :]
        mapped = dot(maps_ref[b], conv_in, tn)
        lru = None
        for d, state_ref in enumerate((before_ref, after_ref)):
            state = state_ref[part, :]
            recur = 1.0 / (1.0 + jnp.exp(-mapped[2 * d * size : (2 * d + 1) * size]))
            inward = 1.0 / (1.0 + jnp.exp(-mapped[(2 * d + 1) * size : (2 * d + 2) * size]))
            speed = speed_ref[part, d : d + 1]
            log_decay = jump - speed * recur
            decay = jnp.exp(log_decay)
            root = jnp.sqrt(one_less_exp(2.0 * log_decay, decay * decay))
            gated = inward * conv
            term = decay * state + root * gated
            lru = term if d == 0 else lru + term
            decay_ref[d, part, :] = decay
            direct_ref[d, part, :] = root * inward
            inward_ref[d, part, :] = root * gated * (1.0 - inward)
            slope = decay * (state - gated * decay / root)
            recur_ref[d, part, :] = -(slope * speed) * (recur * (1.0 - recur))
        x = branch_ref[part, :].astype(f32)
        c = 0.7978845608028654
        t = jnp.tanh(c * (x + 0.044715 * (x * x * x)))
        gelu = 0.5 * x * (1.0 + t)
        slope = 0.5 * (1.0 + t) + 0.5 * x * (1.0 - t * t) * (c * (1.0 + 0.134145 * (x * x)))
        mix_ref[part, :] = (lru * gelu).astype(bf16)
        gelu_ref[part, :] = gelu
        back_ref[part, :] = lru * slope


def project_kernel(ranks, place_ref, mix_ref, *refs):
    parts, out_ref = refs[:ranks], refs[ranks]
    width = parts[0].shape[1]
    across = out_ref.shape[2]
    mix = mix_ref[...]
    for r in range(ranks):
        value = dot(mix, parts[r][...], nn).astype(bf16)
        for j in range(width // across):
            out_ref[(place_ref[0] ^ r) * (width // across) + j] = value[:, j * across : (j + 1) * across]


def scan_kernel(ranks, place_ref, proj_ref, gelu_ref, back_ref, decay_ref, *refs):
    parts = refs[:ranks]
    branch_ref, local_ref, reach_ref, ends_ref, grad_ref = refs[ranks:]
    width = parts[0].shape[1]
    place = place_ref[0]
    total = None
    for r in range(ranks):
        where = pl.ds(pl.multiple_of((place ^ r) * width, width), width)
        one = dot(proj_ref[:, where], parts[r][...], nt)
        total = one if r == 0 else total + one
    grad_ref[...] = total
    channels, length = gelu_ref.shape
    size = min(64, channels)
    for b in range(channels // size):
        part = slice(b * size, (b + 1) * size)
        mix_grad = grad_ref[part, :]
        lru_grad = mix_grad * gelu_ref[part, :]
        branch_ref[part, :] = mix_grad * back_ref[part, :]
        lane = lax.broadcasted_iota(jnp.int32, (size, 128), 1)
        ends = jnp.zeros((size, 128), f32)
        for d in range(2):
            reverse = d == 0
            prod = decay_ref[d, part, :]
            local = prod * lru_grad
            step = 1
            while step < length:
                local = local + prod * shifted(local, step, reverse, 0.0)
                prod = prod * shifted(prod, step, reverse, 1.0)
                step *= 2
            last = slice(0, 1) if reverse else slice(length - 1, length)
            ends = jnp.where(lane == 2 * d, prod[:, last], ends)
            ends = jnp.where(lane == 2 * d + 1, local[:, last], ends)
            local_ref[d, part, :] = lru_grad + shifted(local, 1, reverse, 0.0)
            reach_ref[d, part, :] = shifted(prod, 1, reverse, 1.0)
        ends_ref[:, part] = ends.T[:8]


def finish_kernel(
    place_ref, ends_ref, local_ref, reach_ref, direct_ref, recur_ref, inward_ref, maps_ref, out_ref
):
    count, _, channels = ends_ref.shape
    place = place_ref[0]
    ahead = jnp.zeros((1, channels), f32)
    behind = jnp.zeros((1, channels), f32)
    for e in range(count):
        back = ends_ref[e, 2:3] * behind + ends_ref[e, 3:4]
        behind = jnp.where(e < place, back, behind)
        e = count - 1 - e
        fore = ends_ref[e, 0:1] * ahead + ends_ref[e, 1:2]
        ahead = jnp.where(e > place, fore, ahead)
    row = lax.broadcasted_iota(jnp.int32, (128, channels), 0)
    both = jnp.where(row == 0, ahead, jnp.where(row == 1, behind, 0.0)).T
    blocks, size = maps_ref.shape[0], maps_ref.shape[1]
    for b in range(blocks):
        part = slice(b * size, (b + 1) * size)
        total = None
        stacked = []
        for d in range(2):
            delta = local_ref[d, part, :] + reach_ref[d, part, :] * both[part, d : d + 1]
            direct = delta * direct_ref[d, part, :]
            total = direct if d == 0 else total + direct
            stacked += [delta * recur_ref[d, part, :], delta * inward_ref[d, part, :]]
        wide = jnp.concatenate(stacked, axis=0)
        high = wide.astype(bf16)
        low = (wide - high.astype(f32)).astype(bf16)
        out_ref[part, :] = total + (dot(maps_ref[b], high, nn) + dot(maps_ref[b], low, nn))


def swap(value, axis, bit):
    count = lax.axis_size(axis)
    return lax.ppermute(value, axis, [(i, i ^ bit) for i in range(count)])


def gather_parts(own):
    ranks = lax.axis_size("tp")
    parts = {0: own}
    bit = 2
    while bit < ranks:
        for r in list(parts):
            parts[r | bit] = swap(parts[r], "tp", bit)
        bit *= 2
    if ranks > 1:
        for r in list(parts):
            parts[r | 1] = swap(parts[r], "tp", 1)
    return [parts[r] for r in range(ranks)]


def sum_parts(keep, send):
    got = swap(send, "tp", 1)
    bit = 2
    ranks = lax.axis_size("tp")
    value = keep.astype(f32) + got.astype(f32)
    while bit < ranks:
        half = value.shape[0] // 2
        got = swap(value[half:].astype(bf16), "tp", bit)
        value = value[:half] + got.astype(f32)
        bit *= 2
    return value[0].astype(bf16)


def on_device(
    cotangent, moe_input, routes, gates, w_gate, w_up, w_down, out_proj,
    conv_in, branch, state_before, state_after, jump, recur_weight, input_weight, lam,
):
    tokens, width = cotangent.shape
    top = routes.shape[1]
    experts = lax.axis_size("sp")
    ranks = lax.axis_size("tp")
    capacity = 3 * tokens // experts
    features = width * ranks
    hidden = w_gate.shape[2]
    channels, length = conv_in.shape
    sp = lax.axis_index("sp").astype(jnp.int32).reshape(1)
    tp = lax.axis_index("tp").astype(jnp.int32).reshape(1)

    packed = call(
        functools.partial(pack_kernel, experts, capacity),
        (sp, routes, gates, moe_input, cotangent),
        [shape((tokens, top), jnp.int32)]
        + [shape((capacity, 2 * width), bf16) for _ in range(experts)],
        flops=6 * tokens * experts * capacity * width,
        name="pack",
    )
    positions, blocks = packed[0], packed[1:]

    maps = jnp.stack(
        [recur_weight[0], input_weight[0], recur_weight[1], input_weight[1]], axis=2
    )
    maps = maps.reshape(maps.shape[0], maps.shape[1], -1)
    speed = decay_scale * jax.nn.softplus(-lam).T
    plane = shape((channels, length), f32)
    pair = shape((2, channels, length), f32)
    mix, gelu_val, gelu_back, decay, direct, recur, inward = call(
        gates_kernel,
        (conv_in, branch, state_before, state_after, jump, maps, speed),
        [shape((channels, length), bf16), plane, plane, pair, pair, pair, pair],
        flops=400 * channels * length,
        scalars=0,
        name="gates",
    )

    weights = (w_gate[0], w_up[0], w_down[0])
    count = experts // groups_of_sources
    group_rows = count * capacity
    gathered, hiddens, returned = [], [], [None] * experts
    arrived = [blocks[0]] + [swap(blocks[s], "sp", s) for s in range(1, experts)]
    for g in range(groups_of_sources):
        sources = range(g * count, (g + 1) * count)
        own = jnp.concatenate([arrived[s] for s in sources], axis=0)
        parts = gather_parts(own)
        gathered += parts
        part_kind = shape((ranks // 2, group_rows, width), bf16)
        hid_kind = shape((group_rows, hidden), bf16)
        keep, send, *hids = call(
            functools.partial(expert_kernel, ranks),
            (tp, *parts, *weights),
            [part_kind, part_kind, hid_kind, hid_kind, hid_kind],
            flops=10 * group_rows * features * hidden,
            name="expert",
        )
        hiddens.append(hids)
        row_grad = sum_parts(keep, send)
        for i, s in enumerate(sources):
            block = row_grad[i * capacity : (i + 1) * capacity]
            returned[s] = swap(block, "sp", s) if s else block

    grads = pl.pallas_call(
        functools.partial(weight_kernel, ranks, groups_of_sources),
        out_shape=(
            shape((features, hidden), bf16),
            shape((features, hidden), bf16),
            shape((hidden, features), bf16),
        ),
        in_specs=[pl.BlockSpec(memory_space=pltpu.SMEM)]
        + [pl.BlockSpec(memory_space=pltpu.VMEM)] * (groups_of_sources * (ranks + 3)),
        out_specs=(pl.BlockSpec(memory_space=pl.ANY),) * 3,
        scratch_shapes=[
            pltpu.VMEM((ranks, width, hidden), bf16),
            pltpu.VMEM((ranks, width, hidden), bf16),
            pltpu.VMEM((ranks, hidden, width), bf16),
            pltpu.SemaphoreType.DMA((3, ranks)),
        ],
        cost_estimate=pl.CostEstimate(
            flops=6 * experts * capacity * features * hidden,
            bytes_accessed=6 * features * hidden + 4 * experts * capacity * features,
            transcendentals=0,
        ),
        compiler_params=pltpu.CompilerParams(vmem_limit_bytes=48 * 1024 * 1024),
        name="weights",
    )(tp, *gathered, *[hids[j] for j in range(3) for hids in hiddens])
    gate_grad, up_grad, down_grad = grads

    (residual_grad,) = call(
        functools.partial(combine_kernel, experts),
        (sp, routes, positions, cotangent, *returned),
        [shape((tokens, width), bf16)],
        flops=2 * tokens * experts * capacity * width,
        name="combine",
    )
    parts = gather_parts(residual_grad)
    across = features // experts
    (projected,) = call(
        functools.partial(project_kernel, ranks),
        (tp, mix, *parts),
        [shape((experts, channels, across), bf16)],
        flops=2 * channels * tokens * features,
        name="project",
    )
    branch_grad, local, reach, ends = call(
        functools.partial(scan_kernel, ranks),
        (tp, out_proj, gelu_val, gelu_back, decay, *parts),
        [plane, pair, pair, shape((8, channels), f32)],
        scratch=[pltpu.VMEM((channels, length), f32)],
        flops=2 * channels * tokens * features,
        name="scan",
    )
    all_ends = lax.all_to_all(
        jnp.broadcast_to(ends[None], (experts, *ends.shape)), "sp", 0, 0, tiled=True
    )
    exchanged = lax.all_to_all(projected, "sp", 0, 0, tiled=True)
    (conv_grad,) = call(
        finish_kernel,
        (sp, all_ends, local, reach, direct, recur, inward, maps),
        [plane],
        flops=400 * channels * length,
        name="finish",
    )
    out_proj_grad = jnp.sum(exchanged.astype(f32), axis=0)
    return (
        gate_grad[None], up_grad[None], down_grad[None], residual_grad,
        out_proj_grad, conv_grad, branch_grad,
    )


def solution(mesh):
    placed = (
        P("sp", "tp"), P("sp", "tp"), P("sp", None), P("sp", None),
        P("sp", None, "tp"), P("sp", None, "tp"), P("sp", "tp", None), P("tp", None),
        P("tp", "sp"), P("tp", "sp"), P("tp", "sp"), P("tp", "sp"), P("tp", "sp"),
        P(None, "tp", None, None), P(None, "tp", None, None), P(None, "tp"),
    )
    return jax.shard_map(
        on_device,
        mesh=mesh,
        in_specs=placed,
        out_specs=(
            P("sp", None, "tp"), P("sp", None, "tp"), P("sp", "tp", None), P("sp", "tp"),
            P("tp", "sp"), P("tp", "sp"), P("tp", "sp"),
        ),
        check_vma=False,
    )
```

```python
import functools

import jax
import jax.numpy as jnp
from jax import lax
from jax.experimental import pallas as pl
from jax.experimental.pallas import tpu as pltpu
from jax.sharding import PartitionSpec as P


decay_scale = 8.0
f32 = jnp.float32
bf16 = jnp.bfloat16

nn = (((1,), (0,)), ((), ()))
nt = (((1,), (1,)), ((), ()))
tn = (((0,), (0,)), ((), ()))


def dot(a, b, dims):
    return lax.dot_general(a, b, dims, preferred_element_type=f32)


def call(kernel, inputs, outs, scratch=(), flops=0, scalars=1, grant=12, free=0):
    moved = sum(a.size * a.dtype.itemsize for a in inputs) + sum(
        o.size * o.dtype.itemsize for o in outs
    )
    specs = [pl.BlockSpec(memory_space=pltpu.SMEM)] * scalars
    specs += [pl.BlockSpec(memory_space=pl.ANY)] * free
    specs += [pl.BlockSpec(memory_space=pltpu.VMEM)] * (len(inputs) - scalars - free)
    return pl.pallas_call(
        kernel,
        out_shape=tuple(outs),
        in_specs=specs,
        out_specs=tuple(pl.BlockSpec(memory_space=pltpu.VMEM) for _ in outs),
        scratch_shapes=list(scratch),
        cost_estimate=pl.CostEstimate(
            flops=int(flops), bytes_accessed=int(moved), transcendentals=0
        ),
        compiler_params=pltpu.CompilerParams(vmem_limit_bytes=grant * 1024 * 1024),
    )(*inputs)


def shape(dims, kind):
    return jax.ShapeDtypeStruct(dims, kind)


def pack_kernel(experts, capacity, place_ref, *refs):
    far, out_refs, near, sems = refs[:4], refs[4 : 5 + experts], refs[5 + experts : -1], refs[-1]
    fetches = [
        pltpu.make_async_copy(a, b, sems.at[i]) for i, (a, b) in enumerate(zip(far, near))
    ]
    for fetch in fetches:
        fetch.start()
    routes_ref, gates_ref, rows_ref, cot_ref = near
    position_ref, blocks = out_refs[0], out_refs[1:]
    fetches[0].wait()
    fetches[1].wait()
    top, tokens = routes_ref.shape
    filler = jnp.zeros((8 - 2 * top % 8, tokens), f32)
    table = jnp.concatenate([routes_ref[...].astype(f32), gates_ref[...], filler], axis=0).T
    width = rows_ref.shape[1]
    lanes = max(128, experts)
    named = lax.broadcasted_iota(jnp.int32, (tokens, lanes), 1)
    picks = [table[:, k : k + 1].astype(jnp.int32) for k in range(top)]
    onehots = [(pick == named).astype(f32) for pick in picks]
    both = functools.reduce(jnp.add, onehots).astype(bf16)
    before = (
        lax.broadcasted_iota(jnp.int32, (tokens, tokens), 0)
        > lax.broadcasted_iota(jnp.int32, (tokens, tokens), 1)
    ).astype(f32).astype(bf16)
    earlier = dot(before, both, nn)
    positions = [
        jnp.sum(earlier * onehot, axis=1, keepdims=True).astype(jnp.int32) for onehot in onehots
    ]
    for k in range(top):
        position_ref[:, k : k + 1] = picks[k]
        position_ref[:, top + k : top + k + 1] = positions[k]
    for fetch in fetches[2:]:
        fetch.wait()
    rows = rows_ref[...]
    cot = cot_ref[...].astype(f32)
    scaled = [(cot * table[:, top + k : top + k + 1]).astype(bf16) for k in range(top)]
    slot = lax.broadcasted_iota(jnp.int32, (tokens, capacity), 1)
    for s in range(experts):
        expert = place_ref[0] ^ s
        selects = [
            (jnp.where(pick == expert, position, -1) == slot).astype(f32).astype(bf16)
            for pick, position in zip(picks, positions)
        ]
        blocks[s][:, :width] = dot(functools.reduce(jnp.add, selects), rows, tn).astype(bf16)
        grads = functools.reduce(jnp.add, [dot(sel, sc, tn) for sel, sc in zip(selects, scaled)])
        blocks[s][:, width:] = grads.astype(bf16)


def combine_kernel(experts, place_ref, table_ref, cot_ref, *refs):
    blocks, out_ref = refs[:experts], refs[experts]
    tokens, top = table_ref.shape[0], table_ref.shape[1] // 2
    capacity = blocks[0].shape[0]
    slot = lax.broadcasted_iota(jnp.int32, (tokens, capacity), 1)
    total = cot_ref[...].astype(f32)
    added = jnp.zeros_like(total)
    for s in range(experts):
        expert = place_ref[0] ^ s
        select = functools.reduce(
            jnp.add,
            [
                (
                    jnp.where(
                        table_ref[:, k : k + 1] == expert, table_ref[:, top + k : top + k + 1], -1
                    )
                    == slot
                ).astype(f32)
                for k in range(top)
            ],
        ).astype(bf16)
        added = added + dot(select, blocks[s][...], nn)
    out_ref[...] = (total + added).astype(bf16)


def bit_order(count):
    bits = count.bit_length() - 1
    return [int(format(i, "0%db" % bits)[::-1], 2) if bits else 0 for i in range(count)]


def expert_kernel(ranks, chunks, place_ref, *refs):
    parts = [refs[c * ranks : (c + 1) * ranks] for c in range(chunks)]
    gate_ref, up_ref, down_ref = refs[ranks * chunks : ranks * chunks + 3]
    keep_ref, send_ref, act_ref, gate_hid_ref, up_hid_ref = refs[ranks * chunks + 3 :]
    width = parts[0][0].shape[1] // 2
    hidden = gate_ref.shape[1]
    tile = min(256, hidden)
    place = place_ref[0]
    offsets = [pl.multiple_of((place ^ r) * width, width) for r in range(ranks)]
    for h in range(hidden // tile):
        cols = slice(h * tile, (h + 1) * tile)
        pre_gate = pre_up = act_grad = None
        for r in range(ranks):
            rows = jnp.concatenate([part[r][:, :width] for part in parts], axis=0)
            grads = jnp.concatenate([part[r][:, width:] for part in parts], axis=0)
            where = pl.ds(offsets[r], width)
            one = dot(rows, gate_ref[where, cols], nn)
            two = dot(rows, up_ref[where, cols], nn)
            three = dot(grads, down_ref[cols, where], nt)
            pre_gate = one if r == 0 else pre_gate + one
            pre_up = two if r == 0 else pre_up + two
            act_grad = three if r == 0 else act_grad + three
        sig = 1.0 / (1.0 + jnp.exp(-pre_gate))
        silu = pre_gate * sig
        slope = sig * (1.0 + pre_gate * (1.0 - sig))
        act_ref[:, cols] = (silu * pre_up).astype(bf16)
        up_hid_ref[:, cols] = (act_grad * silu).astype(bf16)
        gate_hid_ref[:, cols] = (act_grad * pre_up * slope).astype(bf16)
    gate_hid = gate_hid_ref[...]
    up_hid = up_hid_ref[...]
    half = ranks // 2
    order = bit_order(ranks)
    for i in [*range(half, ranks), *range(half)]:
        where = pl.ds(offsets[order[i]], width)
        part = dot(gate_hid, gate_ref[where, :], nt) + dot(up_hid, up_ref[where, :], nt)
        if i < half:
            keep_ref[i] = part.astype(bf16)
        else:
            send_ref[i - half] = part.astype(bf16)


def weight_kernel(ranks, chunks, groups, place_ref, *refs):
    parts = [refs[c * ranks : (c + 1) * ranks] for c in range(chunks)]
    rest = refs[chunks * ranks :]
    gate_hids, up_hids = rest[:groups], rest[groups : 2 * groups]
    gate_out, up_out, gate_buf, up_buf, sems = rest[2 * groups :]
    width = parts[0][0].shape[1] // 2
    gate_hid = jnp.concatenate([ref[...] for ref in gate_hids], axis=0)
    up_hid = jnp.concatenate([ref[...] for ref in up_hids], axis=0)
    copies = []
    for r in range(ranks):
        where = pl.ds(pl.multiple_of((place_ref[0] ^ r) * width, width), width)
        rows = jnp.concatenate([part[r][:, :width] for part in parts], axis=0).T
        for j, (hid, buf, out) in enumerate(
            ((gate_hid, gate_buf, gate_out), (up_hid, up_buf, up_out))
        ):
            buf[r] = dot(rows, hid, nn).astype(bf16)
            copies.append(pltpu.make_async_copy(buf.at[r], out.at[where, :], sems.at[j, r]))
            copies[-1].start()
    for copy in copies:
        copy.wait()


def down_kernel(ranks, chunks, groups, place_ref, *refs):
    parts = [refs[c * ranks : (c + 1) * ranks] for c in range(chunks)]
    hids = refs[chunks * ranks : chunks * ranks + groups]
    out, buf, sems = refs[chunks * ranks + groups :]
    width = parts[0][0].shape[1] // 2
    hid = jnp.concatenate([ref[...] for ref in hids], axis=0).T
    copies = []
    for r in range(ranks):
        where = pl.ds(pl.multiple_of((place_ref[0] ^ r) * width, width), width)
        grads = jnp.concatenate([part[r][:, width:] for part in parts], axis=0)
        buf[r] = dot(hid, grads, nn).astype(bf16)
        copies.append(pltpu.make_async_copy(buf.at[r], out.at[:, where], sems.at[r]))
        copies[-1].start()
    for copy in copies:
        copy.wait()


def ticket_kernel(place_ref, out_ref):
    out_ref[0] = place_ref[0]


def ticket(place, flops):
    return pl.pallas_call(
        ticket_kernel,
        out_shape=shape((1,), jnp.int32),
        in_specs=[pl.BlockSpec(memory_space=pltpu.SMEM)],
        out_specs=pl.BlockSpec(memory_space=pltpu.SMEM),
        cost_estimate=pl.CostEstimate(flops=int(flops), bytes_accessed=8, transcendentals=0),
        compiler_params=pltpu.CompilerParams(vmem_limit_bytes=1024 * 1024),
        name="ticket",
    )(place)


def shifted(values, step, reverse, fill):
    length = values.shape[1]
    lane = lax.broadcasted_iota(jnp.int32, values.shape, 1)
    if reverse:
        return jnp.where(lane < length - step, pltpu.roll(values, length - step, 1), fill)
    return jnp.where(lane >= step, pltpu.roll(values, step, 1), fill)


def one_less_exp(power, value):
    series = 1.0 + power * (1.0 / 7.0)
    for term in range(6, 1, -1):
        series = 1.0 + power * (1.0 / term) * series
    return jnp.where(power > -0.35, -power * series, 1.0 - value)


def softplus(value):
    small = jnp.exp(-jnp.abs(value))
    series = 1.0 / 7.0
    for term in range(6, 0, -1):
        series = 1.0 / term - small * series
    return jnp.maximum(value, 0.0) + jnp.where(small < 0.05, small * series, jnp.log(1.0 + small))


def sigmoid(value):
    return 1.0 / (1.0 + jnp.exp(-value))


def gates_kernel(
    recur_maps, input_maps, lam_ref, conv_ref, before_ref, after_ref, jump_ref, branch_ref,
    mix_ref, gelu_ref, back_ref, decay_ref, direct_ref, recur_ref, inward_ref,
):
    blocks, size = recur_maps.shape[1], recur_maps.shape[2]
    channels = blocks * size
    rates = decay_scale * softplus(-lam_ref[...])
    rates = jnp.concatenate([rates, jnp.zeros((6, channels), f32)], axis=0).T
    for b in range(blocks):
        part = slice(b * size, (b + 1) * size)
        conv_in = conv_ref[part, :]
        conv = conv_in.astype(f32)
        jump = jump_ref[part, :]
        lru = None
        for d, state_ref in enumerate((before_ref, after_ref)):
            state = state_ref[part, :]
            recur = sigmoid(dot(recur_maps[d, b], conv_in, tn))
            inward = sigmoid(dot(input_maps[d, b], conv_in, tn))
            speed = rates[part, d : d + 1]
            log_decay = jump - speed * recur
            decay = jnp.exp(log_decay)
            root = jnp.sqrt(one_less_exp(2.0 * log_decay, decay * decay))
            gated = inward * conv
            term = decay * state + root * gated
            lru = term if d == 0 else lru + term
            decay_ref[d, part, :] = decay
            direct_ref[d, part, :] = root * inward
            inward_ref[d, part, :] = root * gated * (1.0 - inward)
            slope = decay * (state - gated * decay / root)
            recur_ref[d, part, :] = -(slope * speed) * (recur * (1.0 - recur))
        x = branch_ref[part, :].astype(f32)
        c = 0.7978845608028654
        t = jnp.tanh(c * (x + 0.044715 * (x * x * x)))
        gelu = 0.5 * x * (1.0 + t)
        slope = 0.5 * (1.0 + t) + 0.5 * x * (1.0 - t * t) * (c * (1.0 + 0.134145 * (x * x)))
        mix_ref[part, :] = (lru * gelu).astype(bf16)
        gelu_ref[part, :] = gelu
        back_ref[part, :] = lru * slope


def project_kernel(ranks, experts, tp_ref, sp_ref, mix_ref, *refs):
    parts, outs, buf = refs[:ranks], refs[ranks : ranks + experts], refs[-1]
    width = parts[0].shape[1]
    across = buf.shape[2]
    mix = mix_ref[...]
    for r in range(ranks):
        value = dot(mix, parts[r][...], nn).astype(bf16)
        for j in range(width // across):
            buf[(tp_ref[0] ^ r) * (width // across) + j] = value[:, j * across : (j + 1) * across]
    for s in range(experts):
        outs[s][...] = buf[sp_ref[0] ^ s]


def scan_kernel(ranks, place_ref, proj_ref, gelu_ref, back_ref, decay_ref, *refs):
    parts = refs[:ranks]
    branch_ref, local_ref, reach_ref, ends_ref, grad_ref = refs[ranks:]
    width = parts[0].shape[1]
    place = place_ref[0]
    total = None
    for r in range(ranks):
        where = pl.ds(pl.multiple_of((place ^ r) * width, width), width)
        one = dot(proj_ref[:, where], parts[r][...], nt)
        total = one if r == 0 else total + one
    grad_ref[...] = total
    channels, length = gelu_ref.shape
    size = min(64, channels)
    for b in range(channels // size):
        part = slice(b * size, (b + 1) * size)
        mix_grad = grad_ref[part, :]
        lru_grad = mix_grad * gelu_ref[part, :]
        branch_ref[part, :] = mix_grad * back_ref[part, :]
        lane = lax.broadcasted_iota(jnp.int32, (size, 128), 1)
        ends = jnp.zeros((size, 128), f32)
        for d in range(2):
            reverse = d == 0
            prod = decay_ref[d, part, :]
            local = prod * lru_grad
            step = 1
            while step < length:
                local = local + prod * shifted(local, step, reverse, 0.0)
                prod = prod * shifted(prod, step, reverse, 1.0)
                step *= 2
            last = slice(0, 1) if reverse else slice(length - 1, length)
            ends = jnp.where(lane == 2 * d, prod[:, last], ends)
            ends = jnp.where(lane == 2 * d + 1, local[:, last], ends)
            local_ref[d, part, :] = lru_grad + shifted(local, 1, reverse, 0.0)
            reach_ref[d, part, :] = shifted(prod, 1, reverse, 1.0)
        ends_ref[:, part] = ends.T[:8]


def finish_kernel(
    place_ref, ends_ref, local_ref, reach_ref, direct_ref, recur_ref, inward_ref,
    recur_maps, input_maps, out_ref,
):
    count, _, channels = ends_ref.shape
    place = place_ref[0]
    ahead = jnp.zeros((1, channels), f32)
    behind = jnp.zeros((1, channels), f32)
    for e in range(count):
        back = ends_ref[e, 2:3] * behind + ends_ref[e, 3:4]
        behind = jnp.where(e < place, back, behind)
        e = count - 1 - e
        fore = ends_ref[e, 0:1] * ahead + ends_ref[e, 1:2]
        ahead = jnp.where(e > place, fore, ahead)
    row = lax.broadcasted_iota(jnp.int32, (128, channels), 0)
    both = jnp.where(row == 0, ahead, jnp.where(row == 1, behind, 0.0)).T
    blocks, size = recur_maps.shape[1], recur_maps.shape[2]
    for b in range(blocks):
        part = slice(b * size, (b + 1) * size)
        total = None
        for d in range(2):
            delta = local_ref[d, part, :] + reach_ref[d, part, :] * both[part, d : d + 1]
            direct = delta * direct_ref[d, part, :]
            total = direct if d == 0 else total + direct
            for maps, slopes in ((recur_maps, recur_ref), (input_maps, inward_ref)):
                wide = delta * slopes[d, part, :]
                high = wide.astype(bf16)
                low = (wide - high.astype(f32)).astype(bf16)
                total = total + (dot(maps[d, b], high, nn) + dot(maps[d, b], low, nn))
        out_ref[part, :] = total


def swap(value, axis, bit):
    count = lax.axis_size(axis)
    return lax.ppermute(value, axis, [(i, i ^ bit) for i in range(count)])


def rank_bits(ranks):
    bits = [1 << b for b in range(1, ranks.bit_length() - 1)]
    return bits + [1] if ranks > 1 else []


def gather_parts(own):
    ranks = lax.axis_size("tp")
    parts = {0: own}
    for bit in rank_bits(ranks):
        for r in list(parts):
            parts[r | bit] = swap(parts[r], "tp", bit)
    return [parts[r] for r in range(ranks)]


def sum_parts(keep, send):
    got = swap(send, "tp", 1)
    ranks = lax.axis_size("tp")
    value = keep.astype(f32) + got.astype(f32)
    bit = 2
    while bit < ranks:
        half = value.shape[0] // 2
        got = swap(value[half:].astype(bf16), "tp", bit)
        value = value[:half] + got.astype(f32)
        if 2 * bit == ranks:
            return value[0].astype(bf16)
        bit *= 2
    return value[0].astype(bf16)


def chunk_plan(experts):
    unit = max(1, experts // 8)
    return [list(range(a, a + unit)) for a in range(0, experts, unit)], [[0, 1], [2, 3], [4, 5], [6, 7]]


def scheduled(
    cotangent, moe_input, routes, gates, w_gate, w_up, w_down, out_proj,
    conv_in, branch, state_before, state_after, jump, recur_weight, input_weight, lam,
):
    tokens, width = cotangent.shape
    top = routes.shape[1]
    experts = lax.axis_size("sp")
    ranks = lax.axis_size("tp")
    capacity = 3 * tokens // experts
    features = width * ranks
    hidden = w_gate.shape[2]
    channels, length = conv_in.shape
    sp = lax.axis_index("sp").astype(jnp.int32).reshape(1)
    tp = lax.axis_index("tp").astype(jnp.int32).reshape(1)

    inputs = (routes.T, gates.T, moe_input, cotangent)
    packed = call(
        functools.partial(pack_kernel, experts, capacity),
        (sp, *inputs),
        [shape((tokens, 2 * top), jnp.int32)]
        + [shape((capacity, 2 * width), bf16) for _ in range(experts)],
        scratch=[pltpu.VMEM(a.shape, a.dtype) for a in inputs]
        + [pltpu.SemaphoreType.DMA((len(inputs),))],
        flops=6 * tokens * experts * capacity * width,
        free=4,
        grant=60,
    )
    table, blocks = packed[0], packed[1:]

    plane = shape((channels, length), f32)
    pair = shape((2, channels, length), f32)
    gate_inputs = (
        recur_weight, input_weight, lam, conv_in, state_before, state_after, jump, branch,
    )
    gate_outs = (shape((channels, length), bf16), plane, plane, pair, pair, pair, pair)
    mix, gelu_val, gelu_back, decay, direct, recur, inward = call(
        gates_kernel, gate_inputs, gate_outs, flops=400 * channels * length, scalars=0, grant=12
    )

    turn = ticket(tp, 40 * tokens * features * hidden)
    weights = (w_gate[0], w_up[0], w_down[0])
    chunks, groups = chunk_plan(experts)
    arrived = [blocks[0]]
    arrived += [swap(blocks[s], "sp", s) for s in range(1, experts)]
    parts = []
    for sources in chunks:
        own = [arrived[s] for s in sources]
        own = own[0] if len(own) == 1 else jnp.concatenate(own, axis=0)
        parts.append(gather_parts(own))
    hiddens, returned = [], [None] * experts
    for members in groups:
        sources = [s for c in members for s in chunks[c]]
        group_rows = len(sources) * capacity
        part_kind = shape((ranks // 2, group_rows, width), bf16)
        hid_kind = shape((group_rows, hidden), bf16)
        keep, send, *hids = call(
            functools.partial(expert_kernel, ranks, len(members)),
            (turn, *[part for c in members for part in parts[c]], *weights),
            [part_kind, part_kind, hid_kind, hid_kind, hid_kind],
            flops=10 * group_rows * features * hidden,
        )
        hiddens.append(hids)
        row_grad = sum_parts(keep, send)
        for i, s in enumerate(sources):
            block = row_grad[i * capacity : (i + 1) * capacity]
            returned[s] = swap(block, "sp", s) if s else block

    every = (tp, *[p for part in parts for p in part])
    sizes = (ranks, len(chunks), len(groups))

    def weight_call(kernel, hids, outs, scratch):
        return pl.pallas_call(
            functools.partial(kernel, *sizes),
            out_shape=tuple(outs),
            in_specs=[pl.BlockSpec(memory_space=pltpu.SMEM)]
            + [pl.BlockSpec(memory_space=pltpu.VMEM)] * (len(every) - 1 + len(hids)),
            out_specs=tuple(pl.BlockSpec(memory_space=pl.ANY) for _ in outs),
            scratch_shapes=[pltpu.VMEM(dims, bf16) for dims in scratch]
            + [pltpu.SemaphoreType.DMA((2, ranks) if len(outs) > 1 else (ranks,))],
            cost_estimate=pl.CostEstimate(
                flops=2 * len(outs) * experts * capacity * features * hidden,
                bytes_accessed=2 * features * (hidden + experts * capacity),
                transcendentals=0,
            ),
            compiler_params=pltpu.CompilerParams(vmem_limit_bytes=16 * 1024 * 1024),
        )(*every, *hids)

    row_dims, col_dims = (features, hidden), (hidden, features)
    gate_grad, up_grad = weight_call(
        weight_kernel,
        [hids[j] for j in (1, 2) for hids in hiddens],
        [shape(row_dims, bf16)] * 2,
        [(ranks, width, hidden)] * 2,
    )
    (down_grad,) = weight_call(
        down_kernel,
        [hids[0] for hids in hiddens],
        [shape(col_dims, bf16)],
        [(ranks, hidden, width)],
    )

    (residual_grad,) = call(
        functools.partial(combine_kernel, experts),
        (sp, table, cotangent, *returned),
        [shape((tokens, width), bf16)],
        flops=2 * tokens * experts * capacity * width,
        grant=12,
    )
    full = gather_parts(residual_grad)
    across = features // experts
    block = shape((channels, across), bf16)
    projected = call(
        functools.partial(project_kernel, ranks, experts),
        (tp, sp, mix, *full),
        [block] * experts,
        scratch=[pltpu.VMEM((experts, channels, across), bf16)],
        flops=2 * channels * tokens * features,
        scalars=2,
        grant=12,
    )
    exchanged = [projected[0]]
    exchanged += [swap(projected[s], "sp", s) for s in range(1, experts)]
    branch_grad, local, reach, ends = call(
        functools.partial(scan_kernel, ranks),
        (tp, out_proj, gelu_val, gelu_back, decay, *full),
        [plane, pair, pair, shape((8, channels), f32)],
        scratch=[pltpu.VMEM((channels, length), f32)],
        flops=2 * channels * tokens * features,
        grant=12,
    )
    all_ends = lax.all_to_all(
        jnp.broadcast_to(ends[None], (experts, *ends.shape)), "sp", 0, 0, tiled=True
    )
    (conv_grad,) = call(
        finish_kernel,
        (sp, all_ends, local, reach, direct, recur, inward, recur_weight, input_weight),
        [plane],
        flops=400 * channels * length,
        grant=12,
    )
    out_proj_grad = functools.reduce(jnp.add, [part.astype(f32) for part in exchanged])
    return (
        gate_grad[None], up_grad[None], down_grad[None], residual_grad,
        out_proj_grad, conv_grad, branch_grad,
    )


def solution(mesh):
    placed = (
        P("sp", "tp"), P("sp", "tp"), P("sp", None), P("sp", None),
        P("sp", None, "tp"), P("sp", None, "tp"), P("sp", "tp", None), P("tp", None),
        P("tp", "sp"), P("tp", "sp"), P("tp", "sp"), P("tp", "sp"), P("tp", "sp"),
        P(None, "tp", None, None), P(None, "tp", None, None), P(None, "tp"),
    )
    return jax.shard_map(
        scheduled,
        mesh=mesh,
        in_specs=placed,
        out_specs=(
            P("sp", None, "tp"), P("sp", None, "tp"), P("sp", "tp", None), P("sp", "tp"),
            P("tp", "sp"), P("tp", "sp"), P("tp", "sp"),
        ),
        check_vma=False,
    )
```

```python
import functools

import jax
import jax.numpy as jnp
from jax import lax
from jax.experimental import pallas as pl
from jax.experimental.pallas import tpu as pltpu
from jax.sharding import PartitionSpec as P


decay_scale = 8.0
f32 = jnp.float32
bf16 = jnp.bfloat16

nn = (((1,), (0,)), ((), ()))
nt = (((1,), (1,)), ((), ()))
tn = (((0,), (0,)), ((), ()))


def dot(a, b, dims):
    return lax.dot_general(a, b, dims, preferred_element_type=f32)


def call(kernel, inputs, outs, scratch=(), flops=0, scalars=1, grant=12, free=0):
    moved = sum(a.size * a.dtype.itemsize for a in inputs) + sum(
        o.size * o.dtype.itemsize for o in outs
    )
    specs = [pl.BlockSpec(memory_space=pltpu.SMEM)] * scalars
    specs += [pl.BlockSpec(memory_space=pl.ANY)] * free
    specs += [pl.BlockSpec(memory_space=pltpu.VMEM)] * (len(inputs) - scalars - free)
    return pl.pallas_call(
        kernel,
        out_shape=tuple(outs),
        in_specs=specs,
        out_specs=tuple(pl.BlockSpec(memory_space=pltpu.VMEM) for _ in outs),
        scratch_shapes=list(scratch),
        cost_estimate=pl.CostEstimate(
            flops=int(flops), bytes_accessed=int(moved), transcendentals=0
        ),
        compiler_params=pltpu.CompilerParams(vmem_limit_bytes=grant * 1024 * 1024),
    )(*inputs)


def shape(dims, kind):
    return jax.ShapeDtypeStruct(dims, kind)


def pack_kernel(experts, capacity, place_ref, *refs):
    far, out_refs, near, sems = refs[:4], refs[4 : 5 + experts], refs[5 + experts : -1], refs[-1]
    fetches = [
        pltpu.make_async_copy(a, b, sems.at[i]) for i, (a, b) in enumerate(zip(far, near))
    ]
    for fetch in fetches:
        fetch.start()
    routes_ref, gates_ref, rows_ref, cot_ref = near
    table_ref, blocks = out_refs[0], out_refs[1:]
    fetches[0].wait()
    top, tokens = routes_ref.shape
    width = rows_ref.shape[1]
    picks = [routes_ref[k : k + 1, :] for k in range(top)]
    named = lax.broadcasted_iota(jnp.int32, (-(-experts // 16) * 16, tokens), 0)
    onehots = [(pick == named).astype(f32) for pick in picks]
    both = functools.reduce(jnp.add, onehots).astype(bf16)
    before = (
        lax.broadcasted_iota(jnp.int32, (tokens, tokens), 0)
        < lax.broadcasted_iota(jnp.int32, (tokens, tokens), 1)
    ).astype(f32).astype(bf16)
    earlier = dot(both, before, nn)
    positions = [jnp.sum(earlier * onehot, axis=0, keepdims=True) for onehot in onehots]
    table_ref[...] = jnp.zeros_like(table_ref)
    for k in range(top):
        table_ref[k : k + 1, :] = picks[k].astype(f32)
        table_ref[top + k : top + k + 1, :] = positions[k]
    for fetch in fetches[1:]:
        fetch.wait()
    both = jnp.concatenate([rows_ref[...], cot_ref[...]], axis=1)
    slot = lax.broadcasted_iota(jnp.int32, (capacity, tokens), 0)
    for s in range(experts):
        expert = place_ref[0] ^ s
        selects = [
            (jnp.where(pick == expert, position.astype(jnp.int32), -1) == slot).astype(f32)
            for pick, position in zip(picks, positions)
        ]
        scales = [sel * gates_ref[k : k + 1, :] for k, sel in enumerate(selects)]
        scale = jnp.sum(functools.reduce(jnp.add, scales), axis=1, keepdims=True)
        moved = dot(functools.reduce(jnp.add, selects).astype(bf16), both, nn)
        blocks[s][:, :width] = moved[:, :width].astype(bf16)
        blocks[s][:, width:] = (moved[:, width:] * scale).astype(bf16)


def combine_kernel(experts, top, place_ref, table_ref, cot_ref, *refs):
    blocks, out_ref = refs[:experts], refs[experts]
    tokens = table_ref.shape[1]
    capacity = blocks[0].shape[0]
    table = table_ref[...].T.astype(jnp.int32)
    slot = lax.broadcasted_iota(jnp.int32, (tokens, capacity), 1)
    total = cot_ref[...].astype(f32)
    added = jnp.zeros_like(total)
    for s in range(experts):
        expert = place_ref[0] ^ s
        select = functools.reduce(
            jnp.add,
            [
                (
                    jnp.where(table[:, k : k + 1] == expert, table[:, top + k : top + k + 1], -1)
                    == slot
                ).astype(f32)
                for k in range(top)
            ],
        ).astype(bf16)
        added = added + dot(select, blocks[s][...], nn)
    out_ref[...] = (total + added).astype(bf16)


def bit_order(count):
    bits = count.bit_length() - 1
    return [int(format(i, "0%db" % bits)[::-1], 2) if bits else 0 for i in range(count)]


def expert_kernel(ranks, chunks, place_ref, *refs):
    parts = [refs[c * ranks : (c + 1) * ranks] for c in range(chunks)]
    gate_ref, up_ref, down_ref = refs[ranks * chunks : ranks * chunks + 3]
    keep_ref, send_ref, act_ref, gate_hid_ref, up_hid_ref = refs[ranks * chunks + 3 :]
    width = parts[0][0].shape[1] // 2
    hidden = gate_ref.shape[1]
    tile = min(256, hidden)
    place = place_ref[0]
    offsets = [pl.multiple_of((place ^ r) * width, width) for r in range(ranks)]
    for h in range(hidden // tile):
        cols = slice(h * tile, (h + 1) * tile)
        pre_gate = pre_up = act_grad = None
        for r in range(ranks):
            rows = jnp.concatenate([part[r][:, :width] for part in parts], axis=0)
            grads = jnp.concatenate([part[r][:, width:] for part in parts], axis=0)
            where = pl.ds(offsets[r], width)
            one = dot(rows, gate_ref[where, cols], nn)
            two = dot(rows, up_ref[where, cols], nn)
            three = dot(grads, down_ref[cols, where], nt)
            pre_gate = one if r == 0 else pre_gate + one
            pre_up = two if r == 0 else pre_up + two
            act_grad = three if r == 0 else act_grad + three
        sig = 1.0 / (1.0 + jnp.exp(-pre_gate))
        silu = pre_gate * sig
        slope = sig * (1.0 + pre_gate * (1.0 - sig))
        act_ref[:, cols] = (silu * pre_up).astype(bf16)
        up_hid_ref[:, cols] = (act_grad * silu).astype(bf16)
        gate_hid_ref[:, cols] = (act_grad * pre_up * slope).astype(bf16)
    gate_hid = gate_hid_ref[...]
    up_hid = up_hid_ref[...]
    half = ranks // 2
    order = bit_order(ranks)
    for i in [*range(half, ranks), *range(half)]:
        where = pl.ds(offsets[order[i]], width)
        part = dot(gate_hid, gate_ref[where, :], nt) + dot(up_hid, up_ref[where, :], nt)
        if i < half:
            keep_ref[i] = part.astype(bf16)
        else:
            send_ref[i - half] = part.astype(bf16)


def weight_kernel(ranks, chunks, groups, place_ref, *refs):
    parts = [refs[c * ranks : (c + 1) * ranks] for c in range(chunks)]
    rest = refs[chunks * ranks :]
    gate_hids, up_hids = rest[:groups], rest[groups : 2 * groups]
    gate_out, up_out, gate_buf, up_buf, sems = rest[2 * groups :]
    width = parts[0][0].shape[1] // 2
    gate_hid = jnp.concatenate([ref[...] for ref in gate_hids], axis=0)
    up_hid = jnp.concatenate([ref[...] for ref in up_hids], axis=0)
    copies = []
    for r in range(ranks):
        where = pl.ds(pl.multiple_of((place_ref[0] ^ r) * width, width), width)
        rows = jnp.concatenate([part[r][:, :width] for part in parts], axis=0).T
        for j, (hid, buf, out) in enumerate(
            ((gate_hid, gate_buf, gate_out), (up_hid, up_buf, up_out))
        ):
            buf[r] = dot(rows, hid, nn).astype(bf16)
            copies.append(pltpu.make_async_copy(buf.at[r], out.at[where, :], sems.at[j, r]))
            copies[-1].start()
    for copy in copies:
        copy.wait()


def down_kernel(ranks, chunks, groups, place_ref, *refs):
    parts = [refs[c * ranks : (c + 1) * ranks] for c in range(chunks)]
    hids = refs[chunks * ranks : chunks * ranks + groups]
    out, buf, sems = refs[chunks * ranks + groups :]
    width = parts[0][0].shape[1] // 2
    hid = jnp.concatenate([ref[...] for ref in hids], axis=0).T
    copies = []
    for r in range(ranks):
        where = pl.ds(pl.multiple_of((place_ref[0] ^ r) * width, width), width)
        grads = jnp.concatenate([part[r][:, width:] for part in parts], axis=0)
        buf[r] = dot(hid, grads, nn).astype(bf16)
        copies.append(pltpu.make_async_copy(buf.at[r], out.at[:, where], sems.at[r]))
        copies[-1].start()
    for copy in copies:
        copy.wait()


def ticket_kernel(place_ref, out_ref):
    out_ref[0] = place_ref[0]


def ticket(place, flops):
    return pl.pallas_call(
        ticket_kernel,
        out_shape=shape((1,), jnp.int32),
        in_specs=[pl.BlockSpec(memory_space=pltpu.SMEM)],
        out_specs=pl.BlockSpec(memory_space=pltpu.SMEM),
        cost_estimate=pl.CostEstimate(flops=int(flops), bytes_accessed=8, transcendentals=0),
        compiler_params=pltpu.CompilerParams(vmem_limit_bytes=1024 * 1024),
        name="ticket",
    )(place)


def shifted(values, step, reverse, fill):
    length = values.shape[1]
    lane = lax.broadcasted_iota(jnp.int32, values.shape, 1)
    if reverse:
        return jnp.where(lane < length - step, pltpu.roll(values, length - step, 1), fill)
    return jnp.where(lane >= step, pltpu.roll(values, step, 1), fill)


def one_less_exp(power, value):
    series = 1.0 + power * (1.0 / 7.0)
    for term in range(6, 1, -1):
        series = 1.0 + power * (1.0 / term) * series
    return jnp.where(power > -0.35, -power * series, 1.0 - value)


def softplus(value):
    small = jnp.exp(-jnp.abs(value))
    series = 1.0 / 7.0
    for term in range(6, 0, -1):
        series = 1.0 / term - small * series
    return jnp.maximum(value, 0.0) + jnp.where(small < 0.05, small * series, jnp.log(1.0 + small))


def sigmoid(value):
    return 1.0 / (1.0 + jnp.exp(-value))


def gates_kernel(
    recur_maps, input_maps, lam_ref, conv_ref, before_ref, after_ref, jump_ref, branch_ref,
    mix_ref, gelu_ref, back_ref, decay_ref, direct_ref, recur_ref, inward_ref,
):
    blocks, size = recur_maps.shape[1], recur_maps.shape[2]
    channels = blocks * size
    rates = decay_scale * softplus(-lam_ref[...])
    rates = jnp.concatenate([rates, jnp.zeros((6, channels), f32)], axis=0).T
    for b in range(blocks):
        part = slice(b * size, (b + 1) * size)
        conv_in = conv_ref[part, :]
        conv = conv_in.astype(f32)
        jump = jump_ref[part, :]
        lru = None
        for d, state_ref in enumerate((before_ref, after_ref)):
            state = state_ref[part, :]
            recur = sigmoid(dot(recur_maps[d, b], conv_in, tn))
            inward = sigmoid(dot(input_maps[d, b], conv_in, tn))
            speed = rates[part, d : d + 1]
            log_decay = jump - speed * recur
            decay = jnp.exp(log_decay)
            root = jnp.sqrt(one_less_exp(2.0 * log_decay, decay * decay))
            gated = inward * conv
            term = decay * state + root * gated
            lru = term if d == 0 else lru + term
            decay_ref[d, part, :] = decay
            direct_ref[d, part, :] = root * inward
            inward_ref[d, part, :] = root * gated * (1.0 - inward)
            slope = decay * (state - gated * decay / root)
            recur_ref[d, part, :] = -(slope * speed) * (recur * (1.0 - recur))
        x = branch_ref[part, :].astype(f32)
        c = 0.7978845608028654
        t = jnp.tanh(c * (x + 0.044715 * (x * x * x)))
        gelu = 0.5 * x * (1.0 + t)
        slope = 0.5 * (1.0 + t) + 0.5 * x * (1.0 - t * t) * (c * (1.0 + 0.134145 * (x * x)))
        mix_ref[part, :] = (lru * gelu).astype(bf16)
        gelu_ref[part, :] = gelu
        back_ref[part, :] = lru * slope


def project_kernel(ranks, experts, tp_ref, sp_ref, mix_ref, *refs):
    parts, outs, buf = refs[:ranks], refs[ranks : ranks + experts], refs[-1]
    width = parts[0].shape[1]
    across = buf.shape[2]
    mix = mix_ref[...]
    for r in range(ranks):
        value = dot(mix, parts[r][...], nn).astype(bf16)
        for j in range(width // across):
            buf[(tp_ref[0] ^ r) * (width // across) + j] = value[:, j * across : (j + 1) * across]
    for s in range(experts):
        outs[s][...] = buf[sp_ref[0] ^ s]


def scan_kernel(ranks, place_ref, proj_ref, gelu_ref, back_ref, decay_ref, *refs):
    parts = refs[:ranks]
    branch_ref, local_ref, reach_ref, ends_ref, grad_ref = refs[ranks:]
    width = parts[0].shape[1]
    place = place_ref[0]
    total = None
    for r in range(ranks):
        where = pl.ds(pl.multiple_of((place ^ r) * width, width), width)
        one = dot(proj_ref[:, where], parts[r][...], nt)
        total = one if r == 0 else total + one
    grad_ref[...] = total
    channels, length = gelu_ref.shape
    size = min(64, channels)
    for b in range(channels // size):
        part = slice(b * size, (b + 1) * size)
        mix_grad = grad_ref[part, :]
        lru_grad = mix_grad * gelu_ref[part, :]
        branch_ref[part, :] = mix_grad * back_ref[part, :]
        lane = lax.broadcasted_iota(jnp.int32, (size, 128), 1)
        ends = jnp.zeros((size, 128), f32)
        for d in range(2):
            reverse = d == 0
            prod = decay_ref[d, part, :]
            local = prod * lru_grad
            step = 1
            while step < length:
                local = local + prod * shifted(local, step, reverse, 0.0)
                prod = prod * shifted(prod, step, reverse, 1.0)
                step *= 2
            last = slice(0, 1) if reverse else slice(length - 1, length)
            ends = jnp.where(lane == 2 * d, prod[:, last], ends)
            ends = jnp.where(lane == 2 * d + 1, local[:, last], ends)
            local_ref[d, part, :] = lru_grad + shifted(local, 1, reverse, 0.0)
            reach_ref[d, part, :] = shifted(prod, 1, reverse, 1.0)
        ends_ref[:, part] = ends.T[:8]


def finish_kernel(
    place_ref, ends_ref, local_ref, reach_ref, direct_ref, recur_ref, inward_ref,
    recur_maps, input_maps, out_ref,
):
    count, _, channels = ends_ref.shape
    place = place_ref[0]
    ahead = jnp.zeros((1, channels), f32)
    behind = jnp.zeros((1, channels), f32)
    for e in range(count):
        back = ends_ref[e, 2:3] * behind + ends_ref[e, 3:4]
        behind = jnp.where(e < place, back, behind)
        e = count - 1 - e
        fore = ends_ref[e, 0:1] * ahead + ends_ref[e, 1:2]
        ahead = jnp.where(e > place, fore, ahead)
    row = lax.broadcasted_iota(jnp.int32, (128, channels), 0)
    both = jnp.where(row == 0, ahead, jnp.where(row == 1, behind, 0.0)).T
    blocks, size = recur_maps.shape[1], recur_maps.shape[2]
    for b in range(blocks):
        part = slice(b * size, (b + 1) * size)
        total = None
        for d in range(2):
            delta = local_ref[d, part, :] + reach_ref[d, part, :] * both[part, d : d + 1]
            direct = delta * direct_ref[d, part, :]
            total = direct if d == 0 else total + direct
            for maps, slopes in ((recur_maps, recur_ref), (input_maps, inward_ref)):
                wide = delta * slopes[d, part, :]
                high = wide.astype(bf16)
                low = (wide - high.astype(f32)).astype(bf16)
                total = total + (dot(maps[d, b], high, nn) + dot(maps[d, b], low, nn))
        out_ref[part, :] = total


def swap(value, axis, bit):
    count = lax.axis_size(axis)
    return lax.ppermute(value, axis, [(i, i ^ bit) for i in range(count)])


def rank_bits(ranks):
    bits = [1 << b for b in range(1, ranks.bit_length() - 1)]
    return bits + [1] if ranks > 1 else []


def gather_parts(own):
    ranks = lax.axis_size("tp")
    parts = {0: own}
    for bit in rank_bits(ranks):
        for r in list(parts):
            parts[r | bit] = swap(parts[r], "tp", bit)
    return [parts[r] for r in range(ranks)]


def sum_parts(keep, send):
    got = swap(send, "tp", 1)
    ranks = lax.axis_size("tp")
    value = keep.astype(f32) + got.astype(f32)
    bit = 2
    while bit < ranks:
        half = value.shape[0] // 2
        got = swap(value[half:].astype(bf16), "tp", bit)
        value = value[:half] + got.astype(f32)
        if 2 * bit == ranks:
            return value[0].astype(bf16)
        bit *= 2
    return value[0].astype(bf16)


def chunk_plan(experts):
    unit = max(1, experts // 8)
    return [list(range(a, a + unit)) for a in range(0, experts, unit)], [[0, 1], [2, 3], [4, 5], [6, 7]]


def scheduled(
    cotangent, moe_input, routes, gates, w_gate, w_up, w_down, out_proj,
    conv_in, branch, state_before, state_after, jump, recur_weight, input_weight, lam,
):
    tokens, width = cotangent.shape
    top = routes.shape[1]
    experts = lax.axis_size("sp")
    ranks = lax.axis_size("tp")
    capacity = 3 * tokens // experts
    features = width * ranks
    hidden = w_gate.shape[2]
    channels, length = conv_in.shape
    sp = lax.axis_index("sp").astype(jnp.int32).reshape(1)
    tp = lax.axis_index("tp").astype(jnp.int32).reshape(1)

    inputs = (routes.T, gates.T, moe_input, cotangent)
    packed = call(
        functools.partial(pack_kernel, experts, capacity),
        (sp, *inputs),
        [shape((-(-2 * top // 8) * 8, tokens), f32)]
        + [shape((capacity, 2 * width), bf16) for _ in range(experts)],
        scratch=[pltpu.VMEM(a.shape, a.dtype) for a in inputs]
        + [pltpu.SemaphoreType.DMA((len(inputs),))],
        flops=6 * tokens * experts * capacity * width,
        free=4,
        grant=60,
    )
    table, blocks = packed[0], packed[1:]

    plane = shape((channels, length), f32)
    pair = shape((2, channels, length), f32)
    gate_inputs = (
        recur_weight, input_weight, lam, conv_in, state_before, state_after, jump, branch,
    )
    gate_outs = (shape((channels, length), bf16), plane, plane, pair, pair, pair, pair)
    mix, gelu_val, gelu_back, decay, direct, recur, inward = call(
        gates_kernel, gate_inputs, gate_outs, flops=400 * channels * length, scalars=0, grant=12
    )

    turn = ticket(tp, 40 * tokens * features * hidden)
    weights = (w_gate[0], w_up[0], w_down[0])
    chunks, groups = chunk_plan(experts)
    arrived = [blocks[0]]
    arrived += [swap(blocks[s], "sp", s) for s in range(1, experts)]
    parts = []
    for sources in chunks:
        own = [arrived[s] for s in sources]
        own = own[0] if len(own) == 1 else jnp.concatenate(own, axis=0)
        parts.append(gather_parts(own))
    hiddens, returned = [], [None] * experts
    for members in groups:
        sources = [s for c in members for s in chunks[c]]
        group_rows = len(sources) * capacity
        part_kind = shape((ranks // 2, group_rows, width), bf16)
        hid_kind = shape((group_rows, hidden), bf16)
        keep, send, *hids = call(
            functools.partial(expert_kernel, ranks, len(members)),
            (turn, *[part for c in members for part in parts[c]], *weights),
            [part_kind, part_kind, hid_kind, hid_kind, hid_kind],
            flops=10 * group_rows * features * hidden,
        )
        hiddens.append(hids)
        row_grad = sum_parts(keep, send)
        for i, s in enumerate(sources):
            block = row_grad[i * capacity : (i + 1) * capacity]
            returned[s] = swap(block, "sp", s) if s else block

    every = (tp, *[p for part in parts for p in part])
    sizes = (ranks, len(chunks), len(groups))

    def weight_call(kernel, hids, outs, scratch):
        return pl.pallas_call(
            functools.partial(kernel, *sizes),
            out_shape=tuple(outs),
            in_specs=[pl.BlockSpec(memory_space=pltpu.SMEM)]
            + [pl.BlockSpec(memory_space=pltpu.VMEM)] * (len(every) - 1 + len(hids)),
            out_specs=tuple(pl.BlockSpec(memory_space=pl.ANY) for _ in outs),
            scratch_shapes=[pltpu.VMEM(dims, bf16) for dims in scratch]
            + [pltpu.SemaphoreType.DMA((2, ranks) if len(outs) > 1 else (ranks,))],
            cost_estimate=pl.CostEstimate(
                flops=2 * len(outs) * experts * capacity * features * hidden,
                bytes_accessed=2 * features * (hidden + experts * capacity),
                transcendentals=0,
            ),
            compiler_params=pltpu.CompilerParams(vmem_limit_bytes=16 * 1024 * 1024),
        )(*every, *hids)

    row_dims, col_dims = (features, hidden), (hidden, features)
    gate_grad, up_grad = weight_call(
        weight_kernel,
        [hids[j] for j in (1, 2) for hids in hiddens],
        [shape(row_dims, bf16)] * 2,
        [(ranks, width, hidden)] * 2,
    )
    (down_grad,) = weight_call(
        down_kernel,
        [hids[0] for hids in hiddens],
        [shape(col_dims, bf16)],
        [(ranks, hidden, width)],
    )

    (residual_grad,) = call(
        functools.partial(combine_kernel, experts, top),
        (sp, table, cotangent, *returned),
        [shape((tokens, width), bf16)],
        flops=2 * tokens * experts * capacity * width,
        grant=12,
    )
    full = gather_parts(residual_grad)
    across = features // experts
    block = shape((channels, across), bf16)
    projected = call(
        functools.partial(project_kernel, ranks, experts),
        (tp, sp, mix, *full),
        [block] * experts,
        scratch=[pltpu.VMEM((experts, channels, across), bf16)],
        flops=2 * channels * tokens * features,
        scalars=2,
        grant=12,
    )
    exchanged = [projected[0]]
    exchanged += [swap(projected[s], "sp", s) for s in range(1, experts)]
    branch_grad, local, reach, ends = call(
        functools.partial(scan_kernel, ranks),
        (tp, out_proj, gelu_val, gelu_back, decay, *full),
        [plane, pair, pair, shape((8, channels), f32)],
        scratch=[pltpu.VMEM((channels, length), f32)],
        flops=2 * channels * tokens * features,
        grant=12,
    )
    all_ends = lax.all_to_all(
        jnp.broadcast_to(ends[None], (experts, *ends.shape)), "sp", 0, 0, tiled=True
    )
    (conv_grad,) = call(
        finish_kernel,
        (sp, all_ends, local, reach, direct, recur, inward, recur_weight, input_weight),
        [plane],
        flops=400 * channels * length,
        grant=12,
    )
    out_proj_grad = functools.reduce(jnp.add, [part.astype(f32) for part in exchanged])
    return (
        gate_grad[None], up_grad[None], down_grad[None], residual_grad,
        out_proj_grad, conv_grad, branch_grad,
    )


def solution(mesh):
    placed = (
        P("sp", "tp"), P("sp", "tp"), P("sp", None), P("sp", None),
        P("sp", None, "tp"), P("sp", None, "tp"), P("sp", "tp", None), P("tp", None),
        P("tp", "sp"), P("tp", "sp"), P("tp", "sp"), P("tp", "sp"), P("tp", "sp"),
        P(None, "tp", None, None), P(None, "tp", None, None), P(None, "tp"),
    )
    return jax.shard_map(
        scheduled,
        mesh=mesh,
        in_specs=placed,
        out_specs=(
            P("sp", None, "tp"), P("sp", None, "tp"), P("sp", "tp", None), P("sp", "tp"),
            P("tp", "sp"), P("tp", "sp"), P("tp", "sp"),
        ),
        check_vma=False,
    )
```
